32 devices in a mesh: kv: 16 (over z, y, x), tp: 2 (over core).
Axes of the slice: x: 2, y: 2, z: 4, core: 2. Of those that a mesh axis runs over, the one named last changes fastest.
Arguments:
- tokens: bfloat16 [16, 4096], P(None, ('kv', 'tp')), may hold values from -12 to 12
- lengths: int32 [16], replicated, may hold values from 1 to 2048, 10922 in all
- attn_gain: bfloat16 [4096], P('kv'), may hold values from 0.099609375 to 1.8984375
- w_query: bfloat16 [4096, 2048], P('kv', 'tp'), may hold values from -0.09375 to 0.09375
- w_key: bfloat16 [4096, 2048], P('kv', 'tp'), may hold values from -0.09375 to 0.09375
- w_value: bfloat16 [4096, 4096], P('kv', 'tp'), may hold values from -0.09375 to 0.09375
- w_gate: bfloat16 [4096, 4096], P('kv', 'tp'), may hold values from -0.09375 to 0.09375
- decay_rate: float32 [32], P('tp'), may hold values from 4.8828125e-05 to 0.05
- key_cache: bfloat16 [16, 2048, 2048], P(None, 'kv', 'tp'), may hold values from -6 to 6
- value_cache: bfloat16 [16, 2048, 4096], P(None, 'kv', 'tp'), may hold values from -6 to 6
- head_gain: bfloat16 [4096], P('tp'), may hold values from 0.099609375 to 1.8984375
- w_output: bfloat16 [4096, 4096], P('tp', 'kv'), may hold values from -0.09375 to 0.09375
- mlp_gain: bfloat16 [4096], replicated, may hold values from 0.099609375 to 1.8984375
- w_up: bfloat16 [4096, 16384], P(None, ('kv', 'tp')), may hold values from -0.09375 to 0.09375
- w_down: bfloat16 [16384, 4096], P(('kv', 'tp')), may hold values from -0.09375 to 0.09375
Outputs:
- layer_out: bfloat16 [16, 4096], P(None, ('kv', 'tp'))
The draws below stay inside these ranges and needn't reach their ends.
Inputs may be any that keep to these rules, and one draw needn't show every extreme that they name: Sequence s has lengths[s] live cache positions, 0 to lengths[s] - 1, and its new token stands at position lengths[s]; the longest fills all 2048 positions.
All inputs are finite; a program needn't handle non-finite values.
Results may differ from the reference program's by a relative error of at most 0.012.
Values may be sent and summed in bfloat16 or wider, within the bound.
A program may use at most 64 MiB of HBM per device.

```python
import math
import jax
import jax.numpy as jnp
import numpy as np
from jax import lax

WIDTH = 4096
HEADS = 32
HEAD_KEY = 64
HEAD_VALUE = 128
MLP_UNITS = 16384
SEQS = 16
CACHE = 2048
GROUP_HEADS = 16
N_TP = 2


def draw_tokens(key, part):
    subkeys = jax.random.split(key, 4)
    column = jnp.arange(WIDTH, dtype=jnp.float32) / WIDTH
    col_scale = 0.5 * jnp.exp(column * jnp.log(6.0)) * jnp.exp(0.3 * jax.random.normal(subkeys[0], (WIDTH,), jnp.float32))
    drawn = col_scale * jax.random.normal(subkeys[3], (SEQS, WIDTH), jnp.float32)
    return jnp.clip(drawn, -12.0, 12.0).astype(jnp.bfloat16)


def draw_decay_rate(key, part):
    subkeys = jax.random.split(key, 3)
    slow_rate = jnp.exp(jax.random.uniform(subkeys[0], (HEADS,), jnp.float32, jnp.log(0.1 / CACHE), jnp.log(2.0 / CACHE)))
    fast_rate = jnp.exp(jax.random.uniform(subkeys[1], (HEADS,), jnp.float32, jnp.log(1.0 / 60.0), jnp.log(1.0 / 20.0)))
    chance = 0.5
    is_fast = jax.random.uniform(subkeys[2], (HEADS,), jnp.float32) < chance
    return jnp.where(is_fast, fast_rate, slow_rate).astype(jnp.float32)


def with_spikes(values, stream_key, source, target, parts, factor):
    owner, partner = [(jnp.arange(values.shape[dim]) // (values.shape[dim] // parts)).reshape([-1 if axis == dim else 1 for axis in range(values.ndim)]) for dim in (source, target)]
    chosen = jax.random.permutation(stream_key, parts)[partner]
    strong = (owner == chosen) | (owner == (partner + parts // 2) % parts)
    return jnp.where(strong, factor * values, values)


def block_levels(rng, shape, pieces, least, largest):
    level = 1.0
    for dim, blocks in pieces:
        heights = jax.random.uniform(jax.random.fold_in(jax.random.fold_in(rng, 6), dim), (blocks,), jnp.float32, least / len(pieces), largest / len(pieces))
        level = level * jnp.repeat(jnp.exp(heights), shape[dim] // blocks).reshape((-1,) + (1,) * (len(shape) - 1 - dim))
    return level


def length_profile(number_of, total, most, lean):
    portions = [(1 << 20) // math.isqrt(rank ** lean) + 1 for rank in range(2, number_of + 1)]
    surplus, counts = total - most - (number_of - 1), [1] * (number_of - 1)
    while surplus > 0:
        candidates = [i for i in range(number_of - 1) if counts[i] < most]
        whole, left = sum([portions[i] for i in candidates]), surplus
        for i in candidates:
            extra = min(most - counts[i], max(1, left * portions[i] // whole), surplus)
            counts[i] = counts[i] + extra
            surplus = surplus - extra
    return np.array([most] + counts)


def ragged(key, count, total, limit, skew):
    if count == 2:
        one = jax.random.randint(key, (), max(1, total - limit), min(limit, total - 1) + 1)
        return jnp.stack([one, total - one])
    sizes = jnp.asarray(length_profile(count, total, limit, skew), jnp.int32)
    couples = (count - 1) // 2
    giver, sink = sizes[1:1 + 2 * couples:2], sizes[2:2 + 2 * couples:2]
    room = jnp.minimum(giver - 1, limit - sink)
    shifted = jax.random.randint(jax.random.fold_in(key, 1), (couples,), 0, 1 << 20) % (room + 1)
    sizes = sizes.at[1:1 + 2 * couples:2].set(giver - shifted).at[2:2 + 2 * couples:2].set(sink + shifted)
    return sizes[jax.random.permutation(jax.random.fold_in(key, 2), count)]


def bell_draw(own_key, dims, deviation, limit, cuts=(), held_as=jnp.bfloat16):
    gain = block_levels(own_key, dims, cuts, -0.22, 0.18) if cuts else 1.0
    values = jax.random.normal(own_key, dims, jnp.float32) * deviation * gain
    return jnp.minimum(jnp.maximum(values, -limit), limit).astype(held_as)


def gaussian_with(key, dims, width, bound, shards, heavy, kind=jnp.bfloat16):
    values = width * jax.random.normal(key, dims, jnp.float32)
    if shards:
        values = values * block_levels(key, dims, shards, -0.22, 0.18)
    return jnp.clip(with_spikes(values, jax.random.fold_in(key, 3), *heavy), -bound, bound).astype(kind)


def setup_inputs(seed: int = 0) -> dict:
    arg_keys = jax.random.split(jax.random.key(seed), 16)
    return {
        "tokens": draw_tokens(jax.random.fold_in(arg_keys[15], 71), 0),
        "lengths": ragged(arg_keys[1], SEQS, SEQS * CACHE // 3, CACHE, 2).astype(jnp.int32),
        "attn_gain": jnp.clip(1.0 + 0.18 * jax.random.normal(arg_keys[2], (WIDTH,), jnp.float32), 0.099609375, 1.8984375).astype(jnp.bfloat16),
        "w_query": bell_draw(arg_keys[3], (WIDTH, HEADS * HEAD_KEY), WIDTH ** -0.5, 0.09375, ((0, 16), (1, 2))),
        "w_key": bell_draw(arg_keys[4], (WIDTH, HEADS * HEAD_KEY), WIDTH ** -0.5, 0.09375, ((0, 16), (1, 2))),
        "w_value": bell_draw(arg_keys[5], (WIDTH, HEADS * HEAD_VALUE), WIDTH ** -0.5, 0.09375, ((0, 16), (1, 2))),
        "w_gate": bell_draw(arg_keys[6], (WIDTH, HEADS * HEAD_VALUE), WIDTH ** -0.5, 0.09375, ((0, 16), (1, 2))),
        "decay_rate": draw_decay_rate(jax.random.fold_in(arg_keys[15], 71), 0),
        "key_cache": bell_draw(arg_keys[8], (SEQS, CACHE, HEADS * HEAD_KEY), 1.0, 6.0, ((1, 16), (2, 2))),
        "value_cache": bell_draw(arg_keys[9], (SEQS, CACHE, HEADS * HEAD_VALUE), 1.0, 6.0, ((1, 16), (2, 2))),
        "head_gain": jnp.clip(1.0 + 0.18 * jax.random.normal(arg_keys[10], (HEADS * HEAD_VALUE,), jnp.float32), 0.099609375, 1.8984375).astype(jnp.bfloat16),
        "w_output": bell_draw(arg_keys[11], (HEADS * HEAD_VALUE, WIDTH), (HEADS * HEAD_VALUE) ** -0.5, 0.09375, ((0, 2), (1, 16))),
        "mlp_gain": jnp.clip(1.0 + 0.18 * jax.random.normal(arg_keys[12], (WIDTH,), jnp.float32), 0.099609375, 1.8984375).astype(jnp.bfloat16),
        "w_up": bell_draw(arg_keys[13], (WIDTH, MLP_UNITS), WIDTH ** -0.5, 0.09375, ((1, 32),)),
        "w_down": gaussian_with(arg_keys[14], (MLP_UNITS, WIDTH), MLP_UNITS ** -0.5, 0.09375, ((0, 32),), (0, 1, 32, 2.75)),
    }


EPS = 1e-05
THETA = 10000.0

def scale_after(inputs, gain_vec, weights):
    scaled = (inputs.astype(jnp.float32) * gain_vec.astype(jnp.float32)).astype(jnp.bfloat16)
    product_sum = jnp.dot(scaled, weights, preferred_element_type=jnp.float32)
    column = jnp.dot(gain_vec[None, :], weights, preferred_element_type=jnp.float32)
    widened = inputs.astype(jnp.float32)
    average = lax.optimization_barrier(jnp.sum(widened, -1, keepdims=True)) / WIDTH
    spread = lax.optimization_barrier(jnp.sum(widened * widened, -1, keepdims=True)) / WIDTH - average * average
    return lax.rsqrt(spread + EPS) * (product_sum - average * column)

def rotate(flattened, position):
    row_count = flattened.shape[0]
    grouped = flattened.reshape(row_count, -1, HEAD_KEY)
    halfway = HEAD_KEY // 2
    inverse = jnp.power(THETA, -jnp.arange(halfway, dtype=jnp.float32) / halfway)
    angles = position.astype(jnp.float32)[:, None] * inverse[None, :]
    cosine = jnp.cos(angles)[:, None, :]
    sine_part = jnp.sin(angles)[:, None, :]
    first_half = grouped[..., :halfway]
    second_half = grouped[..., halfway:]
    turned = jnp.concatenate([first_half * cosine - second_half * sine_part, second_half * cosine + first_half * sine_part], -1)
    return turned.reshape(row_count, -1)

def attend_cache(queries, key_cache, value_cache, lengths, decay_rate):
    places = jnp.arange(CACHE, dtype=jnp.int32)

    def one_sequence(bundle):
        query_row, key_rows, value_rows, length_one = bundle
        key_rows = key_rows.reshape(CACHE, HEADS, HEAD_KEY).astype(jnp.float32)
        value_rows = value_rows.reshape(CACHE, HEADS, HEAD_VALUE).astype(jnp.float32)
        scores = jnp.einsum('hd,jhd->hj', query_row.astype(jnp.float32), key_rows) * HEAD_KEY ** (-0.5)
        distance = jnp.maximum(length_one - places, 0).astype(jnp.float32)
        weights = jnp.where((places < length_one)[None, :], jnp.exp(-decay_rate[:, None] * distance[None, :]), 0.0)
        coefficients = lax.optimization_barrier((scores * weights).astype(jnp.bfloat16)).astype(jnp.float32)
        return jnp.einsum('hj,jhe->he', coefficients, value_rows)
    return lax.map(one_sequence, (queries, key_cache, value_cache, lengths))

def reference(tokens, lengths, attn_gain, w_query, w_key, w_value, w_gate, decay_rate, key_cache, value_cache, head_gain, w_output, mlp_gain, w_up, w_down):
    seq_count = tokens.shape[0]
    query_rows = rotate(scale_after(tokens, attn_gain, w_query), lengths).astype(jnp.bfloat16)
    new_key = rotate(scale_after(tokens, attn_gain, w_key), lengths).astype(jnp.bfloat16)
    new_value = scale_after(tokens, attn_gain, w_value).astype(jnp.bfloat16)
    gate_value = scale_after(tokens, attn_gain, w_gate)
    queries = query_rows.reshape(seq_count, HEADS, HEAD_KEY)
    cached = attend_cache(queries, key_cache, value_cache, lengths, decay_rate)
    own_score = lax.optimization_barrier(jnp.sum(queries.astype(jnp.float32) * new_key.reshape(seq_count, HEADS, HEAD_KEY).astype(jnp.float32), -1)) * HEAD_KEY ** (-0.5)
    retained = cached + own_score[:, :, None] * new_value.reshape(seq_count, HEADS, HEAD_VALUE).astype(jnp.float32)
    centered = retained - lax.optimization_barrier(jnp.mean(retained, -1, keepdims=True))
    normed = centered * lax.rsqrt(lax.optimization_barrier(jnp.mean(centered * centered, -1, keepdims=True)) + EPS) * head_gain.reshape(HEADS, HEAD_VALUE).astype(jnp.float32)
    gated_out = (jax.nn.silu(gate_value) * normed.reshape(seq_count, -1)).astype(jnp.bfloat16)
    group_cols = GROUP_HEADS * HEAD_VALUE
    branch = jnp.zeros((seq_count, WIDTH), jnp.float32)
    for member in range(N_TP):
        piece_out = jnp.dot(gated_out[:, member * group_cols:(member + 1) * group_cols], w_output[member * group_cols:(member + 1) * group_cols], preferred_element_type=jnp.float32).astype(jnp.bfloat16)
        branch = branch + lax.optimization_barrier(piece_out).astype(jnp.float32)
    residual = (tokens.astype(jnp.float32) + branch).astype(jnp.bfloat16)
    hidden = jnp.square(jax.nn.relu(scale_after(residual, mlp_gain, w_up))).astype(jnp.bfloat16)
    layer_out = residual.astype(jnp.float32) + jnp.dot(hidden, w_down, preferred_element_type=jnp.float32)
    return layer_out.astype(jnp.bfloat16)
```

```python
import functools

import jax
import jax.numpy as jnp
from jax import lax
from jax.experimental import pallas as pl
from jax.experimental.pallas import tpu as pltpu
from jax.sharding import PartitionSpec as P

WIDTH = 4096
HEAD_KEY = 64
HEAD_VALUE = 128


EPS = 1e-05
THETA = 10000.0


def rotate(flattened, position):
    row_count = flattened.shape[0]
    grouped = flattened.reshape(row_count, -1, HEAD_KEY)
    halfway = HEAD_KEY // 2
    inverse = jnp.power(THETA, -jnp.arange(halfway, dtype=jnp.float32) / halfway)
    angles = position.astype(jnp.float32)[:, None] * inverse[None, :]
    cosine = jnp.cos(angles)[:, None, :]
    sine_part = jnp.sin(angles)[:, None, :]
    first_half = grouped[..., :halfway]
    second_half = grouped[..., halfway:]
    turned = jnp.concatenate(
        [
            first_half * cosine - second_half * sine_part,
            second_half * cosine + first_half * sine_part,
        ],
        -1,
    )
    return turned.reshape(row_count, -1)


def affine(product_sum, column, average, inverse_std):
    return inverse_std[:, None] * (product_sum - average[:, None] * column[None, :])


def on_device(
    tokens,
    lengths,
    attn_gain,
    w_query,
    w_key,
    w_value,
    w_gate,
    decay_rate,
    key_cache,
    value_cache,
    head_gain,
    w_output,
    mlp_gain,
    w_up,
    w_down,
):
    seq_count = tokens.shape[0]
    head_count = decay_rate.shape[0]
    span_rows = key_cache.shape[1]
    block_cols = lax.all_gather(tokens, "tp", axis=1, tiled=True)
    widened = block_cols.astype(jnp.float32)
    scaled = (widened * attn_gain.astype(jnp.float32)).astype(jnp.bfloat16)
    gain_row = attn_gain[None, :]
    part_query = jnp.dot(scaled, w_query, preferred_element_type=jnp.float32)
    part_key = jnp.dot(scaled, w_key, preferred_element_type=jnp.float32)
    part_value = jnp.dot(scaled, w_value, preferred_element_type=jnp.float32)
    part_gate = jnp.dot(scaled, w_gate, preferred_element_type=jnp.float32)
    col_query = jnp.dot(gain_row, w_query, preferred_element_type=jnp.float32)[0]
    col_key = jnp.dot(gain_row, w_key, preferred_element_type=jnp.float32)[0]
    col_value = jnp.dot(gain_row, w_value, preferred_element_type=jnp.float32)[0]
    col_gate = jnp.dot(gain_row, w_gate, preferred_element_type=jnp.float32)[0]
    (
        sum_query,
        sum_key,
        sum_value,
        sum_gate,
        csum_query,
        csum_key,
        csum_value,
        csum_gate,
        first_moment,
        second_moment,
    ) = lax.psum(
        (
            part_query,
            part_key,
            part_value,
            part_gate,
            col_query,
            col_key,
            col_value,
            col_gate,
            jnp.sum(widened, -1),
            jnp.sum(widened * widened, -1),
        ),
        "kv",
    )
    average = first_moment / WIDTH
    inverse_std = lax.rsqrt(second_moment / WIDTH - average * average + EPS)
    query_rows = rotate(affine(sum_query, csum_query, average, inverse_std), lengths).astype(
        jnp.bfloat16
    )
    new_key = rotate(affine(sum_key, csum_key, average, inverse_std), lengths).astype(jnp.bfloat16)
    new_value = affine(sum_value, csum_value, average, inverse_std).astype(jnp.bfloat16)
    gate_value = affine(sum_gate, csum_gate, average, inverse_std)
    queries = query_rows.reshape(seq_count, head_count, HEAD_KEY)
    keys_local = key_cache.reshape(seq_count, span_rows, head_count, HEAD_KEY)
    values_local = value_cache.reshape(seq_count, span_rows, head_count, HEAD_VALUE)
    scores = jnp.einsum(
        "bhd,bjhd->bhj", queries, keys_local, preferred_element_type=jnp.float32
    ) * HEAD_KEY ** (-0.5)
    places = lax.axis_index("kv") * span_rows + jnp.arange(span_rows, dtype=jnp.int32)
    distance = jnp.maximum(lengths[:, None] - places[None, :], 0).astype(jnp.float32)
    live_mask = (places[None, :] < lengths[:, None])[:, None, :]
    weights = jnp.where(live_mask, jnp.exp(-decay_rate[None, :, None] * distance[:, None, :]), 0.0)
    coefficients = (scores * weights).astype(jnp.bfloat16)
    partial_out = jnp.einsum(
        "bhj,bjhe->bhe", coefficients, values_local, preferred_element_type=jnp.float32
    )
    cached = lax.psum(partial_out, "kv")
    own_score = jnp.sum(
        queries.astype(jnp.float32)
        * new_key.reshape(seq_count, head_count, HEAD_KEY).astype(jnp.float32),
        -1,
    ) * HEAD_KEY ** (-0.5)
    retained = cached + own_score[:, :, None] * new_value.reshape(
        seq_count, head_count, HEAD_VALUE
    ).astype(jnp.float32)
    centered = retained - jnp.mean(retained, -1, keepdims=True)
    normed = (
        centered
        * lax.rsqrt(jnp.mean(centered * centered, -1, keepdims=True) + EPS)
        * head_gain.reshape(head_count, HEAD_VALUE).astype(jnp.float32)
    )
    gated_out = (jax.nn.silu(gate_value) * normed.reshape(seq_count, -1)).astype(jnp.bfloat16)
    partial_branch = jnp.dot(gated_out, w_output, preferred_element_type=jnp.float32)
    branch = lax.psum_scatter(
        partial_branch.astype(jnp.bfloat16), "tp", scatter_dimension=1, tiled=True
    ).astype(jnp.float32)
    own_residual = (tokens.astype(jnp.float32) + branch).astype(jnp.bfloat16)
    piece_wide = lax.all_gather(own_residual, ("kv", "tp"), axis=1, tiled=True).astype(jnp.float32)
    scaled_piece = (piece_wide * mlp_gain.astype(jnp.float32)).astype(jnp.bfloat16)
    totals = (
        jnp.dot(scaled_piece, w_up, preferred_element_type=jnp.float32),
        jnp.sum(piece_wide, -1),
        jnp.sum(piece_wide * piece_wide, -1),
    )
    accumulated, first_sum, second_sum = totals
    mid_average = first_sum / WIDTH
    mid_inverse = lax.rsqrt(second_sum / WIDTH - mid_average * mid_average + EPS)
    column_up = jnp.dot(mlp_gain[None, :], w_up, preferred_element_type=jnp.float32)[0]
    hidden = jnp.square(
        jax.nn.relu(affine(accumulated, column_up, mid_average, mid_inverse))
    ).astype(jnp.bfloat16)
    down_terms = jnp.dot(hidden, w_down, preferred_element_type=jnp.float32)
    kv_block = lax.psum_scatter(down_terms, "kv", scatter_dimension=1, tiled=True)
    mixer_sum = lax.psum_scatter(kv_block, "tp", scatter_dimension=1, tiled=True)
    return (own_residual.astype(jnp.float32) + mixer_sum).astype(jnp.bfloat16)


LANES = 128
F32 = jnp.float32
BF16 = jnp.bfloat16


def remote(src, dst, send_sem, recv_sem, device):
    return pltpu.make_async_remote_copy(
        src_ref=src,
        dst_ref=dst,
        send_sem=send_sem,
        recv_sem=recv_sem,
        device_id=device,
        device_id_type=pl.DeviceIdType.MESH,
    )


def turn(x, cosine, sine):
    lane = lax.broadcasted_iota(jnp.int32, x.shape, 1)
    half = HEAD_KEY // 2
    ahead = pltpu.roll(x, LANES - half, 1)
    behind = pltpu.roll(x, half, 1)
    return x * cosine + jnp.where(lane % HEAD_KEY < half, ahead, behind) * sine


def layer_kernel(
    n_kv,
    n_tp,
    width,
    lengths,
    tokens,
    attn_gain,
    cosines,
    sines,
    decay,
    head_gain,
    mlp_gain,
    w_query,
    w_key,
    w_value,
    w_gate,
    key_cache,
    value_cache,
    w_output,
    w_up,
    w_down,
    out,
    wq,
    wk,
    wv,
    wg,
    keys,
    values,
    wo,
    wu,
    wd,
    lhs,
    tok_in,
    q_out,
    q_in,
    qr_out,
    qr_in,
    p_out,
    p_in,
    c_out,
    c_in,
    g_out,
    g_in,
    g_wide,
    g_lhs,
    b_out,
    b_in,
    r_out,
    r_in,
    up_lhs,
    d_out,
    d_in,
    load_sem,
    tok_sem,
    q_sem,
    qr_sem,
    p_sem,
    c_sem,
    g_sem,
    b_sem,
    r_sem,
    d_sem,
):
    count = n_kv * n_tp
    kv = lax.axis_index("kv")
    tp = lax.axis_index("tp")
    me = kv * n_tp + tp
    seqs = tokens.shape[0]
    heads = head_gain.shape[0]
    q_rows = q_out.shape[1]
    span = keys.shape[1]

    pairs = (
        (w_query, wq),
        (w_key, wk),
        (w_value, wv),
        (w_gate, wg),
        (key_cache, keys),
        (value_cache, values),
        (w_output, wo),
        (w_up, wu),
        (w_down, wd),
    )
    loads = [pltpu.make_async_copy(a, b, load_sem.at[i]) for i, (a, b) in enumerate(pairs)]
    for load in loads:
        load.start()

    def other(d):
        return lax.rem(kv + d // n_tp, n_kv), lax.rem(tp + lax.rem(d, n_tp), n_tp)

    def kv_other(d):
        return lax.rem(kv + d, n_kv)

    barrier = pltpu.get_barrier_semaphore()

    def greet(d, carry):
        pl.semaphore_signal(
            barrier, inc=1, device_id=other(d), device_id_type=pl.DeviceIdType.MESH
        )
        return carry

    lax.fori_loop(1, count, greet, 0)
    pl.semaphore_wait(barrier, count - 1)

    def all_copy(src, dst, sems, d):
        a, b = other(d)
        slot = a * n_tp + b
        return remote(src(slot), dst.at[me], sems.at[0, slot], sems.at[1, me], (a, b))

    def all_send(src, dst, sems):
        def body(d, carry):
            all_copy(src, dst, sems, d).start()
            return carry

        lax.fori_loop(1, count, body, 0)

    def all_recv(dst, sems, low, high):
        def body(d, carry):
            a, b = other(d)
            slot = a * n_tp + b
            remote(
                dst.at[slot], dst.at[slot], sems.at[0, slot], sems.at[1, slot], (a, b)
            ).wait_recv()
            return carry

        lax.fori_loop(low, high, body, 0)

    def all_drain(src, dst, sems):
        def body(d, carry):
            all_copy(src, dst, sems, d).wait_send()
            return carry

        lax.fori_loop(1, count, body, 0)

    def kv_copy(src, dst, sems, d):
        a = kv_other(d)
        return remote(src(a), dst.at[kv], sems.at[0, a], sems.at[1, kv], (a, tp))

    def kv_send(src, dst, sems):
        def body(d, carry):
            kv_copy(src, dst, sems, d).start()
            return carry

        lax.fori_loop(1, n_kv, body, 0)

    def kv_recv(dst, sems):
        def body(d, carry):
            a = kv_other(d)
            remote(dst.at[a], dst.at[a], sems.at[0, a], sems.at[1, a], (a, tp)).wait_recv()
            return carry

        lax.fori_loop(1, n_kv, body, 0)

    def kv_drain(src, dst, sems):
        def body(d, carry):
            kv_copy(src, dst, sems, d).wait_send()
            return carry

        lax.fori_loop(1, n_kv, body, 0)

    def tokens_src(slot):
        return tokens

    all_send(tokens_src, tok_in, tok_sem)
    tok_in[me] = tokens[...]
    row = lax.broadcasted_iota(jnp.int32, (seqs, LANES), 0)
    lane = lax.broadcasted_iota(jnp.int32, (seqs, LANES), 1)
    all_recv(tok_in, tok_sem, 1, n_tp)
    for t in range(n_tp):
        cols = slice(t * LANES, (t + 1) * LANES)
        gain = attn_gain[:, cols]
        lhs[:seqs, cols] = (tok_in[kv * n_tp + t].astype(F32) * gain).astype(BF16)
        lhs[seqs:, cols] = jnp.where(row == 0, gain, 0.0).astype(BF16)
    loads[0].wait()
    first = jnp.dot(lhs[...], wq[...], preferred_element_type=F32)
    all_recv(tok_in, tok_sem, n_tp, count)

    def moments(blocks):
        wide = blocks.astype(F32)
        average = jnp.sum(jnp.sum(wide, 0), -1, keepdims=True) / width
        square = jnp.sum(jnp.sum(wide * wide, 0), -1, keepdims=True) / width
        return average, lax.rsqrt(square - average * average + EPS)

    average, inverse = moments(tok_in[...])

    def spread(product, dst, base):
        part = inverse * (product[:seqs] - average * product[seqs : seqs + 1])
        for c in range(part.shape[1] // LANES):
            dst[:, base + c, :] = part[:, c * LANES : (c + 1) * LANES]

    spread(first, q_out, 0)
    kv_send(lambda a: q_out.at[a], q_in, q_sem)
    q_in[kv] = q_out[kv]

    base = 0
    for which, weight in ((1, wk), (2, wv), (3, wg)):
        loads[which].wait()
        for low in range(0, weight.shape[1], 1024):
            high = min(low + 1024, weight.shape[1])
            spread(
                jnp.dot(lhs[...], weight[:, low:high], preferred_element_type=F32), p_out, base
            )
            base += (high - low) // LANES
    p_in[kv] = p_out[kv]

    cosine = cosines[pl.ds(kv, 1), :]
    sine = sines[pl.ds(kv, 1), :]
    kv_recv(q_in, q_sem)
    query = turn(jnp.sum(q_in[...], 0), cosine, sine).astype(BF16).astype(F32)
    qr_out[...] = query
    qr_in[kv] = query
    kv_send(lambda a: qr_out, qr_in, qr_sem)
    kv_send(lambda a: p_out.at[a], p_in, p_sem)

    loads[4].wait()
    loads[5].wait()
    kv_recv(qr_in, qr_sem)
    per_row = LANES // HEAD_KEY
    head_row = lax.broadcasted_iota(jnp.int32, (heads, LANES), 0)
    head_lane = lax.broadcasted_iota(jnp.int32, (heads, LANES), 1)
    place = kv * span + lax.broadcasted_iota(jnp.int32, (1, span), 1)

    def attend(i, carry):
        s = lax.rem(kv + 1 + i, n_kv)
        rows = qr_in[s]
        pieces = [
            jnp.where(
                head_row == per_row * r + head_lane // HEAD_KEY,
                jnp.broadcast_to(rows[r : r + 1], (heads, LANES)),
                0.0,
            )
            for r in range(q_rows)
        ]
        blocked = jnp.concatenate(pieces, 1).astype(BF16)
        scores = lax.dot_general(
            blocked, keys[s], (((1,), (1,)), ((), ())), preferred_element_type=F32
        ) * HEAD_KEY ** (-0.5)
        length = lengths[s]
        distance = jnp.maximum(length - place, 0).astype(F32)
        fade = jnp.where(place < length, jnp.exp(-decay[...] * distance), 0.0)
        coefficients = (scores * fade).astype(BF16)
        mixed = jnp.dot(coefficients, values[s], preferred_element_type=F32)
        kept = jnp.zeros((heads, LANES), F32)
        for h in range(heads):
            kept = jnp.where(head_row == h, mixed[:, h * LANES : (h + 1) * LANES], kept)
        c_out[s] = kept

        @pl.when(i < n_kv - 1)
        def _():
            kv_copy(lambda a: c_out.at[a], c_in, c_sem, 1 + i).start()

        return carry

    lax.fori_loop(0, n_kv, attend, 0)
    c_in[kv] = c_out[kv]

    kv_recv(p_in, p_sem)
    totals = jnp.sum(p_in[...], 0)
    fresh_key = turn(totals[:q_rows], cosine, sine).astype(BF16).astype(F32)
    fresh_value = totals[q_rows : q_rows + heads].astype(BF16).astype(F32)
    gate = totals[q_rows + heads :]
    product = query * fresh_key
    laid = jnp.zeros((heads, LANES), F32)
    for r in range(q_rows):
        laid = jnp.where(
            head_row == per_row * r + head_lane // HEAD_KEY,
            jnp.broadcast_to(product[r : r + 1], (heads, LANES)),
            laid,
        )
    own_score = jnp.sum(laid, -1, keepdims=True) * HEAD_KEY ** (-0.5)
    addend = own_score * fresh_value
    gate = gate * jax.nn.sigmoid(gate)

    kv_recv(c_in, c_sem)
    retained = jnp.sum(c_in[...], 0) + addend
    centered = retained - jnp.mean(retained, -1, keepdims=True)
    normed = (
        centered
        * lax.rsqrt(jnp.mean(centered * centered, -1, keepdims=True) + EPS)
        * head_gain[...]
    )
    gated = (gate * normed).astype(BF16)
    g_out[...] = gated
    g_in[kv] = gated
    kv_send(lambda a: g_out, g_in, g_sem)

    loads[6].wait()
    kv_recv(g_in, g_sem)
    g_wide[...] = g_in[...].astype(F32)
    for h in range(heads):
        g_lhs[:, h * LANES : (h + 1) * LANES] = g_wide[:, h, :].astype(BF16)
    branch = jnp.dot(g_lhs[...], wo[...], preferred_element_type=F32).astype(BF16)
    for t in range(n_tp):
        b_out[t] = branch[:, t * LANES : (t + 1) * LANES]

    def tp_copy(d):
        b = lax.rem(tp + d, n_tp)
        return remote(b_out.at[b], b_in.at[tp], b_sem.at[0, b], b_sem.at[1, tp], (kv, b))

    for d in range(1, n_tp):
        tp_copy(d).start()
    b_in[tp] = b_out[tp]
    for d in range(1, n_tp):
        b = lax.rem(tp + d, n_tp)
        remote(b_in.at[b], b_in.at[b], b_sem.at[0, b], b_sem.at[1, b], (kv, b)).wait_recv()
    residual = (tokens[...].astype(F32) + jnp.sum(b_in[...].astype(F32), 0)).astype(BF16)
    r_out[...] = residual
    r_in[me] = residual

    def residual_src(slot):
        return r_out

    all_send(residual_src, r_in, r_sem)
    loads[7].wait()
    loads[8].wait()
    for j in range(count):
        cols = slice(j * LANES, (j + 1) * LANES)
        up_lhs[seqs:, cols] = jnp.where(row == 0, mlp_gain[:, cols], 0.0).astype(BF16)
    all_recv(r_in, r_sem, 1, count)
    for j in range(count):
        cols = slice(j * LANES, (j + 1) * LANES)
        up_lhs[:seqs, cols] = (r_in[j].astype(F32) * mlp_gain[:, cols]).astype(BF16)
    mid_average, mid_inverse = moments(r_in[...])
    lifted = jnp.dot(up_lhs[...], wu[...], preferred_element_type=F32)
    hidden = jnp.maximum(
        mid_inverse * (lifted[:seqs] - mid_average * lifted[seqs : seqs + 1]), 0.0
    )
    hidden = (hidden * hidden).astype(BF16)
    per_dot = 8
    for low in range(0, count, per_dot):
        high = min(low + per_dot, count)
        lowered = jnp.dot(
            hidden, wd[:, low * LANES : high * LANES], preferred_element_type=F32
        )
        for j in range(low, high):
            d_out[j] = lowered[:, (j - low) * LANES : (j - low + 1) * LANES]
    all_send(lambda slot: d_out.at[slot], d_in, d_sem)
    d_in[me] = d_out[me]

    all_drain(tokens_src, tok_in, tok_sem)
    kv_drain(lambda a: q_out.at[a], q_in, q_sem)
    kv_drain(lambda a: qr_out, qr_in, qr_sem)
    kv_drain(lambda a: p_out.at[a], p_in, p_sem)
    kv_drain(lambda a: c_out.at[a], c_in, c_sem)
    kv_drain(lambda a: g_out, g_in, g_sem)
    for d in range(1, n_tp):
        tp_copy(d).wait_send()
    all_drain(residual_src, r_in, r_sem)
    all_recv(d_in, d_sem, 1, count)
    out[...] = (residual.astype(F32) + jnp.sum(d_in[...], 0)).astype(BF16)
    all_drain(lambda slot: d_out.at[slot], d_in, d_sem)


def on_device_fused(n_kv, n_tp, *args):
    (
        tokens,
        lengths,
        attn_gain,
        w_query,
        w_key,
        w_value,
        w_gate,
        decay_rate,
        key_cache,
        value_cache,
        head_gain,
        w_output,
        mlp_gain,
        w_up,
        w_down,
    ) = args
    seqs, block = tokens.shape
    heads = decay_rate.shape[0]
    count = n_kv * n_tp
    fits = (
        seqs == n_kv
        and block == LANES
        and HEAD_VALUE == LANES
        and heads % 8 == 0
        and count <= 64
        and w_output.shape[1] == n_tp * LANES
    )
    if not fits:
        return on_device(*args)
    half = HEAD_KEY // 2
    turn_rate = jnp.power(THETA, -jnp.arange(half, dtype=F32) / half)
    angles = lengths.astype(F32)[:, None] * turn_rate[None, :]
    cosines = jnp.tile(jnp.cos(angles), (1, LANES // half))
    sine = jnp.sin(angles)
    sines = jnp.tile(jnp.concatenate([-sine, sine], 1), (1, LANES // HEAD_KEY))
    span = key_cache.shape[1]
    decay = jnp.broadcast_to(decay_rate[:, None], (heads, span))
    q_rows = w_query.shape[1] // LANES
    p_rows = q_rows + 2 * heads
    small = pl.BlockSpec(memory_space=pltpu.VMEM)
    large = pl.BlockSpec(memory_space=pl.ANY)
    weights = (
        w_query, w_key, w_value, w_gate, key_cache, value_cache, w_output, w_up, w_down
    )
    vmem = pltpu.VMEM
    dma = pltpu.SemaphoreType.DMA
    return pl.pallas_call(
        functools.partial(layer_kernel, n_kv, n_tp, block * count),
        out_shape=jax.ShapeDtypeStruct((seqs, block), BF16),
        in_specs=[pl.BlockSpec(memory_space=pltpu.SMEM)] + [small] * 7 + [large] * 9,
        out_specs=small,
        scratch_shapes=[vmem(w.shape, w.dtype) for w in weights]
        + [
            vmem((2 * seqs, n_tp * LANES), BF16),
            vmem((count, seqs, LANES), BF16),
            vmem((n_kv, q_rows, LANES), F32),
            vmem((n_kv, q_rows, LANES), F32),
            vmem((q_rows, LANES), F32),
            vmem((n_kv, q_rows, LANES), F32),
            vmem((n_kv, p_rows, LANES), F32),
            vmem((n_kv, p_rows, LANES), F32),
            vmem((n_kv, heads, LANES), F32),
            vmem((n_kv, heads, LANES), F32),
            vmem((heads, LANES), BF16),
            vmem((n_kv, heads, LANES), BF16),
            vmem((n_kv, heads, LANES), F32),
            vmem((seqs, heads * LANES), BF16),
            vmem((n_tp, seqs, LANES), BF16),
            vmem((n_tp, seqs, LANES), BF16),
            vmem((seqs, LANES), BF16),
            vmem((count, seqs, LANES), BF16),
            vmem((2 * seqs, count * LANES), BF16),
            vmem((count, seqs, LANES), F32),
            vmem((count, seqs, LANES), F32),
            dma((len(weights),)),
            dma((2, count)),
            dma((2, n_kv)),
            dma((2, n_kv)),
            dma((2, n_kv)),
            dma((2, n_kv)),
            dma((2, n_kv)),
            dma((2, n_tp)),
            dma((2, count)),
            dma((2, count)),
        ],
        compiler_params=pltpu.CompilerParams(
            collective_id=0, has_side_effects=True, vmem_limit_bytes=56 * 1024 * 1024
        ),
    )(
        lengths,
        tokens,
        attn_gain.astype(F32).reshape(1, -1),
        cosines,
        sines,
        decay,
        head_gain.astype(F32).reshape(heads, LANES),
        mlp_gain.astype(F32).reshape(1, -1),
        *weights,
    )


def solution(mesh):
    in_specs = (
        P(None, ("kv", "tp")),
        P(),
        P("kv"),
        P("kv", "tp"),
        P("kv", "tp"),
        P("kv", "tp"),
        P("kv", "tp"),
        P("tp"),
        P(None, "kv", "tp"),
        P(None, "kv", "tp"),
        P("tp"),
        P("tp", "kv"),
        P(),
        P(None, ("kv", "tp")),
        P(("kv", "tp"), None),
    )
    out_specs = P(None, ("kv", "tp"))
    body = functools.partial(on_device_fused, mesh.shape["kv"], mesh.shape["tp"])
    return jax.shard_map(
        body, mesh=mesh, in_specs=in_specs, out_specs=out_specs, check_vma=False
    )
```

```python
import functools

import jax
import jax.numpy as jnp
from jax import lax
from jax.experimental import pallas as pl
from jax.experimental.pallas import tpu as pltpu
from jax.sharding import PartitionSpec as P

WIDTH = 4096
HEAD_KEY = 64
HEAD_VALUE = 128


EPS = 1e-05
THETA = 10000.0


def rotate(flattened, position):
    row_count = flattened.shape[0]
    grouped = flattened.reshape(row_count, -1, HEAD_KEY)
    halfway = HEAD_KEY // 2
    inverse = jnp.power(THETA, -jnp.arange(halfway, dtype=jnp.float32) / halfway)
    angles = position.astype(jnp.float32)[:, None] * inverse[None, :]
    cosine = jnp.cos(angles)[:, None, :]
    sine_part = jnp.sin(angles)[:, None, :]
    first_half = grouped[..., :halfway]
    second_half = grouped[..., halfway:]
    turned = jnp.concatenate(
        [
            first_half * cosine - second_half * sine_part,
            second_half * cosine + first_half * sine_part,
        ],
        -1,
    )
    return turned.reshape(row_count, -1)


def affine(product_sum, column, average, inverse_std):
    return inverse_std[:, None] * (product_sum - average[:, None] * column[None, :])


def on_device(
    tokens,
    lengths,
    attn_gain,
    w_query,
    w_key,
    w_value,
    w_gate,
    decay_rate,
    key_cache,
    value_cache,
    head_gain,
    w_output,
    mlp_gain,
    w_up,
    w_down,
):
    seq_count = tokens.shape[0]
    head_count = decay_rate.shape[0]
    span_rows = key_cache.shape[1]
    block_cols = lax.all_gather(tokens, "tp", axis=1, tiled=True)
    widened = block_cols.astype(jnp.float32)
    scaled = (widened * attn_gain.astype(jnp.float32)).astype(jnp.bfloat16)
    gain_row = attn_gain[None, :]
    part_query = jnp.dot(scaled, w_query, preferred_element_type=jnp.float32)
    part_key = jnp.dot(scaled, w_key, preferred_element_type=jnp.float32)
    part_value = jnp.dot(scaled, w_value, preferred_element_type=jnp.float32)
    part_gate = jnp.dot(scaled, w_gate, preferred_element_type=jnp.float32)
    col_query = jnp.dot(gain_row, w_query, preferred_element_type=jnp.float32)[0]
    col_key = jnp.dot(gain_row, w_key, preferred_element_type=jnp.float32)[0]
    col_value = jnp.dot(gain_row, w_value, preferred_element_type=jnp.float32)[0]
    col_gate = jnp.dot(gain_row, w_gate, preferred_element_type=jnp.float32)[0]
    (
        sum_query,
        sum_key,
        sum_value,
        sum_gate,
        csum_query,
        csum_key,
        csum_value,
        csum_gate,
        first_moment,
        second_moment,
    ) = lax.psum(
        (
            part_query,
            part_key,
            part_value,
            part_gate,
            col_query,
            col_key,
            col_value,
            col_gate,
            jnp.sum(widened, -1),
            jnp.sum(widened * widened, -1),
        ),
        "kv",
    )
    average = first_moment / WIDTH
    inverse_std = lax.rsqrt(second_moment / WIDTH - average * average + EPS)
    query_rows = rotate(affine(sum_query, csum_query, average, inverse_std), lengths).astype(
        jnp.bfloat16
    )
    new_key = rotate(affine(sum_key, csum_key, average, inverse_std), lengths).astype(jnp.bfloat16)
    new_value = affine(sum_value, csum_value, average, inverse_std).astype(jnp.bfloat16)
    gate_value = affine(sum_gate, csum_gate, average, inverse_std)
    queries = query_rows.reshape(seq_count, head_count, HEAD_KEY)
    keys_local = key_cache.reshape(seq_count, span_rows, head_count, HEAD_KEY)
    values_local = value_cache.reshape(seq_count, span_rows, head_count, HEAD_VALUE)
    scores = jnp.einsum(
        "bhd,bjhd->bhj", queries, keys_local, preferred_element_type=jnp.float32
    ) * HEAD_KEY ** (-0.5)
    places = lax.axis_index("kv") * span_rows + jnp.arange(span_rows, dtype=jnp.int32)
    distance = jnp.maximum(lengths[:, None] - places[None, :], 0).astype(jnp.float32)
    live_mask = (places[None, :] < lengths[:, None])[:, None, :]
    weights = jnp.where(live_mask, jnp.exp(-decay_rate[None, :, None] * distance[:, None, :]), 0.0)
    coefficients = (scores * weights).astype(jnp.bfloat16)
    partial_out = jnp.einsum(
        "bhj,bjhe->bhe", coefficients, values_local, preferred_element_type=jnp.float32
    )
    cached = lax.psum(partial_out, "kv")
    own_score = jnp.sum(
        queries.astype(jnp.float32)
        * new_key.reshape(seq_count, head_count, HEAD_KEY).astype(jnp.float32),
        -1,
    ) * HEAD_KEY ** (-0.5)
    retained = cached + own_score[:, :, None] * new_value.reshape(
        seq_count, head_count, HEAD_VALUE
    ).astype(jnp.float32)
    centered = retained - jnp.mean(retained, -1, keepdims=True)
    normed = (
        centered
        * lax.rsqrt(jnp.mean(centered * centered, -1, keepdims=True) + EPS)
        * head_gain.reshape(head_count, HEAD_VALUE).astype(jnp.float32)
    )
    gated_out = (jax.nn.silu(gate_value) * normed.reshape(seq_count, -1)).astype(jnp.bfloat16)
    partial_branch = jnp.dot(gated_out, w_output, preferred_element_type=jnp.float32)
    branch = lax.psum_scatter(
        partial_branch.astype(jnp.bfloat16), "tp", scatter_dimension=1, tiled=True
    ).astype(jnp.float32)
    own_residual = (tokens.astype(jnp.float32) + branch).astype(jnp.bfloat16)
    piece_wide = lax.all_gather(own_residual, ("kv", "tp"), axis=1, tiled=True).astype(jnp.float32)
    scaled_piece = (piece_wide * mlp_gain.astype(jnp.float32)).astype(jnp.bfloat16)
    totals = (
        jnp.dot(scaled_piece, w_up, preferred_element_type=jnp.float32),
        jnp.sum(piece_wide, -1),
        jnp.sum(piece_wide * piece_wide, -1),
    )
    accumulated, first_sum, second_sum = totals
    mid_average = first_sum / WIDTH
    mid_inverse = lax.rsqrt(second_sum / WIDTH - mid_average * mid_average + EPS)
    column_up = jnp.dot(mlp_gain[None, :], w_up, preferred_element_type=jnp.float32)[0]
    hidden = jnp.square(
        jax.nn.relu(affine(accumulated, column_up, mid_average, mid_inverse))
    ).astype(jnp.bfloat16)
    down_terms = jnp.dot(hidden, w_down, preferred_element_type=jnp.float32)
    kv_block = lax.psum_scatter(down_terms, "kv", scatter_dimension=1, tiled=True)
    mixer_sum = lax.psum_scatter(kv_block, "tp", scatter_dimension=1, tiled=True)
    return (own_residual.astype(jnp.float32) + mixer_sum).astype(jnp.bfloat16)


LANES = 128
F32 = jnp.float32
BF16 = jnp.bfloat16


def remote(src, dst, send_sem, recv_sem, device):
    return pltpu.make_async_remote_copy(
        src_ref=src,
        dst_ref=dst,
        send_sem=send_sem,
        recv_sem=recv_sem,
        device_id=device,
        device_id_type=pl.DeviceIdType.MESH,
    )


def turn(x, cosine, sine):
    lane = lax.broadcasted_iota(jnp.int32, x.shape, 1)
    half = HEAD_KEY // 2
    ahead = pltpu.roll(x, LANES - half, 1)
    behind = pltpu.roll(x, half, 1)
    return x * cosine + jnp.where(lane % HEAD_KEY < half, ahead, behind) * sine


def layer_kernel(
    n_kv,
    n_tp,
    width,
    lengths,
    decay_rate,
    tokens,
    attn_gain,
    head_gain,
    mlp_gain,
    w_query,
    w_key,
    w_value,
    w_gate,
    key_cache,
    value_cache,
    w_output,
    w_up,
    w_down,
    out,
    wq,
    wk,
    wv,
    wg,
    keys,
    values,
    wo,
    wu,
    wd,
    lhs,
    tok_in,
    m_out,
    m_in,
    q_out,
    q_in,
    qr_out,
    qr_in,
    p_wide,
    p_out,
    p_in,
    c_out,
    c_in,
    g_out,
    g_in,
    g_wide,
    g_lhs,
    b_out,
    b_in,
    r_out,
    r_in,
    up_lhs,
    d_out,
    d_in,
    load_sem,
    tok_sem,
    m_sem,
    q_sem,
    qr_sem,
    p_sem,
    c_sem,
    g_sem,
    b_sem,
    r_sem,
    d_sem,
):
    count = n_kv * n_tp
    kv = lax.axis_index("kv")
    tp = lax.axis_index("tp")
    me = kv * n_tp + tp
    seqs = tokens.shape[0]
    heads = head_gain.shape[0]
    q_rows = q_out.shape[1] // 2
    span = keys.shape[1]

    pairs = (
        (w_query, wq),
        (w_key, wk),
        (w_value, wv),
        (w_gate, wg),
        (key_cache, keys),
        (value_cache, values),
        (w_output, wo),
        (w_up, wu),
        (w_down, wd),
    )
    loads = [pltpu.make_async_copy(a, b, load_sem.at[i]) for i, (a, b) in enumerate(pairs)]
    for load in loads:
        load.start()

    def other(d):
        return lax.rem(kv + d // n_tp, n_kv), lax.rem(tp + lax.rem(d, n_tp), n_tp)

    def kv_other(d):
        return lax.rem(kv + d, n_kv)

    barrier = pltpu.get_barrier_semaphore()

    def greet(d, carry):
        pl.semaphore_signal(
            barrier, inc=1, device_id=other(d), device_id_type=pl.DeviceIdType.MESH
        )
        return carry

    lax.fori_loop(1, count, greet, 0)
    pl.semaphore_wait(barrier, count - 1)

    def all_copy(src, dst, sems, d):
        a, b = other(d)
        slot = a * n_tp + b
        return remote(src(slot), dst.at[me], sems.at[0, slot], sems.at[1, me], (a, b))

    def all_send(src, dst, sems):
        def body(d, carry):
            all_copy(src, dst, sems, d).start()
            return carry

        lax.fori_loop(1, count, body, 0)

    def all_recv(dst, sems, low, high):
        def body(d, carry):
            a, b = other(d)
            slot = a * n_tp + b
            remote(
                dst.at[slot], dst.at[slot], sems.at[0, slot], sems.at[1, slot], (a, b)
            ).wait_recv()
            return carry

        lax.fori_loop(low, high, body, 0)

    def all_drain(src, dst, sems):
        def body(d, carry):
            all_copy(src, dst, sems, d).wait_send()
            return carry

        lax.fori_loop(1, count, body, 0)

    def kv_copy(src, dst, sems, d):
        a = kv_other(d)
        return remote(src(a), dst.at[kv], sems.at[0, a], sems.at[1, kv], (a, tp))

    def kv_send(src, dst, sems):
        def body(d, carry):
            kv_copy(src, dst, sems, d).start()
            return carry

        lax.fori_loop(1, n_kv, body, 0)

    def kv_recv(dst, sems):
        def body(d, carry):
            a = kv_other(d)
            remote(dst.at[a], dst.at[a], sems.at[0, a], sems.at[1, a], (a, tp)).wait_recv()
            return carry

        lax.fori_loop(1, n_kv, body, 0)

    def kv_drain(src, dst, sems):
        def body(d, carry):
            kv_copy(src, dst, sems, d).wait_send()
            return carry

        lax.fori_loop(1, n_kv, body, 0)

    def tokens_src(slot):
        return tokens

    def tokens_send(low, high):
        def body(d, carry):
            all_copy(tokens_src, tok_in, tok_sem, d).start()
            return carry

        lax.fori_loop(low, high, body, 0)

    tokens_send(1, n_tp)
    tok_in[me] = tokens[...]
    row = lax.broadcasted_iota(jnp.int32, (seqs, LANES), 0)
    lane = lax.broadcasted_iota(jnp.int32, (seqs, LANES), 1)
    gains = attn_gain[...].astype(F32)
    for t in range(n_tp):
        cols = slice(t * LANES, (t + 1) * LANES)
        lhs[seqs:, cols] = jnp.where(row == 0, gains[t : t + 1], 0.0).astype(BF16)
    all_recv(tok_in, tok_sem, 1, n_tp)
    first_sum = jnp.zeros((seqs, 1), F32)
    second_sum = jnp.zeros((seqs, 1), F32)
    for t in range(n_tp):
        cols = slice(t * LANES, (t + 1) * LANES)
        block = tok_in[kv * n_tp + t].astype(F32)
        lhs[:seqs, cols] = (block * gains[t : t + 1]).astype(BF16)
        first_sum += jnp.sum(block, -1, keepdims=True)
        second_sum += jnp.sum(block * block, -1, keepdims=True)
    m_out[:, 0, :] = jnp.where(lane < LANES // 2, first_sum, second_sum)
    loads[0].wait()
    product = jnp.dot(lhs[...], wq[...], preferred_element_type=F32)
    for c in range(q_rows):
        cols = slice(c * LANES, (c + 1) * LANES)
        q_out[:, c, :] = product[:seqs, cols]
        q_out[:, q_rows + c, :] = jnp.broadcast_to(
            product[seqs : seqs + 1, cols], (seqs, LANES)
        )
    kv_send(lambda a: m_out.at[a], m_in, m_sem)
    kv_send(lambda a: q_out.at[a], q_in, q_sem)
    tokens_send(n_tp, count)
    m_in[kv] = m_out[kv]
    q_in[kv] = q_out[kv]

    lane_row = lax.broadcasted_iota(jnp.int32, (1, LANES), 1)
    half = HEAD_KEY // 2
    turn_rate = jnp.zeros((1, LANES), F32)
    for i in range(half):
        turn_rate = jnp.where(lane_row % half == i, THETA ** (-i / half), turn_rate)
    angle = lengths[kv].astype(F32) * turn_rate
    cosine = jnp.cos(angle)
    sine = jnp.sin(angle)
    sine = jnp.where(lane_row % HEAD_KEY < half, -sine, sine)
    decay = jnp.zeros((heads, LANES), F32)
    for h in range(heads):
        decay = jnp.where(
            lax.broadcasted_iota(jnp.int32, (heads, LANES), 0) == h, decay_rate[h], decay
        )

    def normalizer(first, second):
        average = first / width
        return average, lax.rsqrt(second / width - average * average + EPS)

    def moments(blocks):
        wide = blocks.astype(F32)
        return normalizer(
            jnp.sum(jnp.sum(wide, 0), -1, keepdims=True),
            jnp.sum(jnp.sum(wide * wide, 0), -1, keepdims=True),
        )

    kv_recv(m_in, m_sem)
    sums = jnp.sum(m_in[...], 0)
    own_average, own_inverse = normalizer(sums[:, :1], sums[:, LANES - 1 :])
    kv_recv(q_in, q_sem)
    total = jnp.sum(q_in[...], 0)
    query = own_inverse * (total[:q_rows] - own_average * total[q_rows:])
    query = turn(query, cosine, sine).astype(BF16)
    qr_out[...] = query
    qr_in[kv] = query
    query = query.astype(F32)
    kv_send(lambda a: qr_out, qr_in, qr_sem)

    all_recv(tok_in, tok_sem, n_tp, count)
    average, inverse = moments(tok_in[...])
    base = 0
    for which, weight in ((1, wk), (2, wv), (3, wg)):
        loads[which].wait()
        for low in range(0, weight.shape[1], 1024):
            high = min(low + 1024, weight.shape[1])
            product = jnp.dot(lhs[...], weight[:, low:high], preferred_element_type=F32)
            part = inverse * (product[:seqs] - average * product[seqs : seqs + 1])
            for c in range(part.shape[1] // LANES):
                p_wide[:, base + c, :] = part[:, c * LANES : (c + 1) * LANES]
            base += (high - low) // LANES
    p_out[...] = p_wide[...].astype(BF16)
    p_in[kv] = p_out[kv]
    kv_send(lambda a: p_out.at[a], p_in, p_sem)

    loads[4].wait()
    loads[5].wait()
    kv_recv(qr_in, qr_sem)
    per_row = LANES // HEAD_KEY
    head_row = lax.broadcasted_iota(jnp.int32, (heads, LANES), 0)
    head_lane = lax.broadcasted_iota(jnp.int32, (heads, LANES), 1)
    place = kv * span + lax.broadcasted_iota(jnp.int32, (1, span), 1)

    group = 4 if n_kv % 4 == 0 else 1
    where_lane = [head_row == per_row * r + head_lane // HEAD_KEY for r in range(q_rows)]

    def attend(step, carry):
        order = [lax.rem(kv + 1 + step * group + k, n_kv) for k in range(group)]
        coefficients = []
        for s in order:
            rows = qr_in[s].astype(F32)
            pieces = [
                jnp.where(
                    where_lane[r], jnp.broadcast_to(rows[r : r + 1], (heads, LANES)), 0.0
                )
                for r in range(q_rows)
            ]
            blocked = jnp.concatenate(pieces, 1).astype(BF16)
            scores = lax.dot_general(
                blocked, keys[s], (((1,), (1,)), ((), ())), preferred_element_type=F32
            ) * HEAD_KEY ** (-0.5)
            length = lengths[s]
            distance = jnp.maximum(length - place, 0).astype(F32)
            fade = jnp.where(place < length, jnp.exp(-decay[:, :1] * distance), 0.0)
            coefficients.append((scores * fade).astype(BF16))
        for s, coefficient in zip(order, coefficients):
            mixed = jnp.dot(coefficient, values[s], preferred_element_type=F32)
            kept = jnp.zeros((heads, LANES), F32)
            for h in range(heads):
                kept = jnp.where(head_row == h, mixed[:, h * LANES : (h + 1) * LANES], kept)
            c_out[s] = kept.astype(BF16)
        for k in range(group):
            d = 1 + step * group + k

            @pl.when(d < n_kv)
            def _():
                kv_copy(lambda a: c_out.at[a], c_in, c_sem, d).start()

        return carry

    lax.fori_loop(0, n_kv // group, attend, 0)
    c_in[kv] = c_out[kv]

    kv_recv(p_in, p_sem)
    totals = jnp.sum(p_in[...].astype(F32), 0)
    fresh_key = turn(totals[:q_rows], cosine, sine).astype(BF16).astype(F32)
    fresh_value = totals[q_rows : q_rows + heads].astype(BF16).astype(F32)
    gate = totals[q_rows + heads :]
    product = query * fresh_key
    laid = jnp.zeros((heads, LANES), F32)
    for r in range(q_rows):
        laid = jnp.where(
            head_row == per_row * r + head_lane // HEAD_KEY,
            jnp.broadcast_to(product[r : r + 1], (heads, LANES)),
            laid,
        )
    own_score = jnp.sum(laid, -1, keepdims=True) * HEAD_KEY ** (-0.5)
    addend = own_score * fresh_value
    gate = gate * jax.nn.sigmoid(gate)

    kv_recv(c_in, c_sem)
    retained = jnp.sum(c_in[...].astype(F32), 0) + addend
    centered = retained - jnp.mean(retained, -1, keepdims=True)
    normed = (
        centered
        * lax.rsqrt(jnp.mean(centered * centered, -1, keepdims=True) + EPS)
        * head_gain[...].astype(F32)
    )
    gated = (gate * normed).astype(BF16)
    g_out[...] = gated
    g_in[kv] = gated
    kv_send(lambda a: g_out, g_in, g_sem)

    loads[6].wait()
    kv_recv(g_in, g_sem)
    g_wide[...] = g_in[...].astype(F32)
    for h in range(heads):
        g_lhs[:, h * LANES : (h + 1) * LANES] = g_wide[:, h, :].astype(BF16)
    branch = jnp.dot(g_lhs[...], wo[...], preferred_element_type=F32).astype(BF16)
    for t in range(n_tp):
        b_out[t] = branch[:, t * LANES : (t + 1) * LANES]

    def tp_copy(d):
        b = lax.rem(tp + d, n_tp)
        return remote(b_out.at[b], b_in.at[tp], b_sem.at[0, b], b_sem.at[1, tp], (kv, b))

    for d in range(1, n_tp):
        tp_copy(d).start()
    b_in[tp] = b_out[tp]
    for d in range(1, n_tp):
        b = lax.rem(tp + d, n_tp)
        remote(b_in.at[b], b_in.at[b], b_sem.at[0, b], b_sem.at[1, b], (kv, b)).wait_recv()
    residual = (tokens[...].astype(F32) + jnp.sum(b_in[...].astype(F32), 0)).astype(BF16)
    r_out[...] = residual
    r_in[me] = residual

    def residual_src(slot):
        return r_out

    all_send(residual_src, r_in, r_sem)
    loads[7].wait()
    loads[8].wait()
    gains = mlp_gain[...].astype(F32)
    for j in range(count):
        cols = slice(j * LANES, (j + 1) * LANES)
        up_lhs[seqs:, cols] = jnp.where(row == 0, gains[j : j + 1], 0.0).astype(BF16)
    all_recv(r_in, r_sem, 1, count)
    for j in range(count):
        cols = slice(j * LANES, (j + 1) * LANES)
        up_lhs[:seqs, cols] = (r_in[j].astype(F32) * gains[j : j + 1]).astype(BF16)
    mid_average, mid_inverse = moments(r_in[...])
    lifted = jnp.dot(up_lhs[...], wu[...], preferred_element_type=F32)
    hidden = jnp.maximum(
        mid_inverse * (lifted[:seqs] - mid_average * lifted[seqs : seqs + 1]), 0.0
    )
    hidden = (hidden * hidden).astype(BF16)
    per_dot = 8 if count % 8 == 0 else 1
    chunks = count // per_dot
    for i in range(chunks):
        low = lax.rem(me // per_dot + 1 + i, chunks) * per_dot
        cols = pl.ds(pl.multiple_of(low * LANES, LANES * per_dot), LANES * per_dot)
        lowered = jnp.dot(hidden, wd[:, cols], preferred_element_type=F32)
        for k in range(per_dot):
            d_out[low + k] = lowered[:, k * LANES : (k + 1) * LANES].astype(BF16)
        for k in range(per_dot):
            slot = low + lax.rem(me + k, per_dot)

            @pl.when(slot != me)
            def _():
                remote(
                    d_out.at[slot],
                    d_in.at[me],
                    d_sem.at[0, slot],
                    d_sem.at[1, me],
                    (slot // n_tp, lax.rem(slot, n_tp)),
                ).start()

    d_in[me] = d_out[me]

    all_drain(tokens_src, tok_in, tok_sem)
    kv_drain(lambda a: m_out.at[a], m_in, m_sem)
    kv_drain(lambda a: q_out.at[a], q_in, q_sem)
    kv_drain(lambda a: qr_out, qr_in, qr_sem)
    kv_drain(lambda a: p_out.at[a], p_in, p_sem)
    kv_drain(lambda a: c_out.at[a], c_in, c_sem)
    kv_drain(lambda a: g_out, g_in, g_sem)
    for d in range(1, n_tp):
        tp_copy(d).wait_send()
    all_drain(residual_src, r_in, r_sem)
    all_recv(d_in, d_sem, 1, count)
    out[...] = (residual.astype(F32) + jnp.sum(d_in[...].astype(F32), 0)).astype(BF16)
    all_drain(lambda slot: d_out.at[slot], d_in, d_sem)


def on_device_fused(n_kv, n_tp, *args):
    (
        tokens,
        lengths,
        attn_gain,
        w_query,
        w_key,
        w_value,
        w_gate,
        decay_rate,
        key_cache,
        value_cache,
        head_gain,
        w_output,
        mlp_gain,
        w_up,
        w_down,
    ) = args
    seqs, block = tokens.shape
    heads = decay_rate.shape[0]
    count = n_kv * n_tp
    fits = (
        seqs == n_kv
        and block == LANES
        and HEAD_VALUE == LANES
        and heads % 8 == 0
        and count <= 64
        and w_output.shape[1] == n_tp * LANES
    )
    if not fits:
        return on_device(*args)
    q_rows = w_query.shape[1] // LANES
    p_rows = q_rows + 2 * heads
    small = pl.BlockSpec(memory_space=pltpu.VMEM)
    large = pl.BlockSpec(memory_space=pl.ANY)
    weights = (
        w_query, w_key, w_value, w_gate, key_cache, value_cache, w_output, w_up, w_down
    )
    vmem = pltpu.VMEM
    dma = pltpu.SemaphoreType.DMA
    return pl.pallas_call(
        functools.partial(layer_kernel, n_kv, n_tp, block * count),
        out_shape=jax.ShapeDtypeStruct((seqs, block), BF16),
        in_specs=[pl.BlockSpec(memory_space=pltpu.SMEM)] * 2 + [small] * 4 + [large] * 9,
        out_specs=small,
        scratch_shapes=[vmem(w.shape, w.dtype) for w in weights]
        + [
            vmem((2 * seqs, n_tp * LANES), BF16),
            vmem((count, seqs, LANES), BF16),
            vmem((n_kv, 1, LANES), F32),
            vmem((n_kv, 1, LANES), F32),
            vmem((n_kv, 2 * q_rows, LANES), F32),
            vmem((n_kv, 2 * q_rows, LANES), F32),
            vmem((q_rows, LANES), BF16),
            vmem((n_kv, q_rows, LANES), BF16),
            vmem((n_kv, p_rows, LANES), F32),
            vmem((n_kv, p_rows, LANES), BF16),
            vmem((n_kv, p_rows, LANES), BF16),
            vmem((n_kv, heads, LANES), BF16),
            vmem((n_kv, heads, LANES), BF16),
            vmem((heads, LANES), BF16),
            vmem((n_kv, heads, LANES), BF16),
            vmem((n_kv, heads, LANES), F32),
            vmem((seqs, heads * LANES), BF16),
            vmem((n_tp, seqs, LANES), BF16),
            vmem((n_tp, seqs, LANES), BF16),
            vmem((seqs, LANES), BF16),
            vmem((count, seqs, LANES), BF16),
            vmem((2 * seqs, count * LANES), BF16),
            vmem((count, seqs, LANES), BF16),
            vmem((count, seqs, LANES), BF16),
            dma((len(weights),)),
            dma((2, count)),
            dma((2, n_kv)),
            dma((2, n_kv)),
            dma((2, n_kv)),
            dma((2, n_kv)),
            dma((2, n_kv)),
            dma((2, n_kv)),
            dma((2, n_tp)),
            dma((2, count)),
            dma((2, count)),
        ],
        compiler_params=pltpu.CompilerParams(
            collective_id=0, has_side_effects=True, vmem_limit_bytes=56 * 1024 * 1024
        ),
    )(
        lengths,
        decay_rate,
        tokens,
        attn_gain.reshape(n_tp, LANES),
        head_gain.reshape(heads, LANES),
        mlp_gain.reshape(count, LANES),
        *weights,
    )


def solution(mesh):
    in_specs = (
        P(None, ("kv", "tp")),
        P(),
        P("kv"),
        P("kv", "tp"),
        P("kv", "tp"),
        P("kv", "tp"),
        P("kv", "tp"),
        P("tp"),
        P(None, "kv", "tp"),
        P(None, "kv", "tp"),
        P("tp"),
        P("tp", "kv"),
        P(),
        P(None, ("kv", "tp")),
        P(("kv", "tp"), None),
    )
    out_specs = P(None, ("kv", "tp"))
    body = functools.partial(on_device_fused, mesh.shape["kv"], mesh.shape["tp"])
    return jax.shard_map(
        body, mesh=mesh, in_specs=in_specs, out_specs=out_specs, check_vma=False
    )
```
